128 devices in a mesh: ra: 16 (over z, x), cb: 8 (over y, core).
Axes of the slice: x: 4, y: 4, z: 4, core: 2. Of those that a mesh axis runs over, the one named last changes fastest.
Arguments:
- inputs: bfloat16 [1536, 4096], P(None, 'ra'), may hold values from -12 to 12
- gate_weight: bfloat16 [2, 4096, 11264], P(None, 'ra', 'cb'), may hold values from -0.09375 to 0.09375
- up_weight: bfloat16 [2, 4096, 11264], P(None, 'ra', 'cb'), may hold values from -0.09375 to 0.09375
- down_weight: bfloat16 [2, 11264, 4096], P(None, 'cb', 'ra'), may hold values from -0.0546875 to 0.0546875
- norm_gain: float32 [2, 4096], P(None, 'ra'), may hold values from 0.05 to 8
- norm_shift: float32 [2, 4096], P(None, 'ra'), may hold values from -1.5 to 1.5
Outputs:
- outputs: bfloat16 [1536, 4096], P(None, 'ra')
The draws below stay inside these ranges and needn't reach their ends.
All inputs are finite; a program needn't handle non-finite values.
Results may differ from the reference program's by a relative error of at most 0.04.
Values may be sent and summed in bfloat16 or wider, within the bound.
No kernel may reach another device: no remote copies, remote signals or barrier semaphores. Data moves between devices by JAX's collectives and lax.ppermute only.
A program may use at most 64 MiB of HBM per device.

```python
import jax
import jax.numpy as jnp
from jax import lax

D = 4096
FF = 11264
TOKENS = 1536
LAYERS = 2
N_RA = 16


def draw_inputs(key, part):
    key = jax.random.fold_in(key, 11)
    keys = jax.random.split(key, 3)
    groups = 32
    factor = jnp.exp(jax.random.uniform(keys[0], (1, groups), jnp.float32, jnp.log(0.3), jnp.log(3.0)))
    offset = jax.random.uniform(keys[1], (1, groups), jnp.float32, -1.0, 1.0)
    factor = jnp.repeat(factor, D // groups, axis=1)
    offset = jnp.repeat(offset, D // groups, axis=1)
    base = jax.random.normal(keys[2], (TOKENS, D), jnp.float32)
    return jnp.clip(base * factor + offset, -12.0, 12.0).astype(jnp.bfloat16)


def draw_norm_gain(key, part):
    key = jax.random.fold_in(key, 23)
    keys = jax.random.split(key, 2)
    groups = 32
    factor = jnp.exp(jax.random.uniform(keys[0], (LAYERS, groups), jnp.float32, jnp.log(0.35), jnp.log(3.0)))
    factor = jnp.repeat(factor, D // groups, axis=1)
    noise = jnp.clip(jax.random.normal(keys[1], (LAYERS, D), jnp.float32), -3.0, 3.0)
    return (factor * (1.0 + 0.18 * noise)).astype(jnp.float32)


def block_levels(stream_key, dims, pieces, low, high):
    level, own = 1.0, jax.random.fold_in(stream_key, 6)
    for axis_at, blocks in pieces:
        draws = jnp.exp(jax.random.uniform(jax.random.fold_in(own, axis_at), (blocks,), jnp.float32, low / len(pieces), high / len(pieces)))
        level = level * jnp.repeat(draws, dims[axis_at] // blocks).reshape([-1 if axis == axis_at else 1 for axis in range(len(dims))])
    return level


def scatter_about(key, shape, spread, most, pieces=(), dtype=jnp.bfloat16):
    loudness = block_levels(key, shape, pieces, -0.22, 0.18) if pieces else 1.0
    entries = jax.random.normal(key, shape, jnp.float32) * spread * loudness
    return jnp.minimum(jnp.maximum(entries, -most), most).astype(dtype)


def setup_inputs(seed: int = 0) -> dict:
    seeds = jax.random.split(jax.random.key(seed), 7)
    inputs = draw_inputs(jax.random.fold_in(seeds[6], 71), 0)
    gate_weight = scatter_about(seeds[1], (LAYERS, D, FF), D ** -0.5, 0.09375, ((1, 16), (2, 8)))
    up_weight = scatter_about(seeds[2], (LAYERS, D, FF), D ** -0.5, 0.09375, ((1, 16), (2, 8)))
    down_weight = scatter_about(seeds[3], (LAYERS, FF, D), FF ** -0.5, 0.0546875, ((1, 8), (2, 16)))
    norm_gain = draw_norm_gain(jax.random.fold_in(seeds[6], 71), 0)
    norm_shift = scatter_about(seeds[5], (LAYERS, D), 0.3, 1.5, ((1, 16),), jnp.float32)
    return {"inputs": inputs, "gate_weight": gate_weight, "up_weight": up_weight, "down_weight": down_weight, "norm_gain": norm_gain, "norm_shift": norm_shift}


RESIDUAL = 0.5
EPSILON = 1e-05

def block_products(stream, paired):
    width = D // N_RA
    total = jnp.zeros((stream.shape[0], paired.shape[1]), jnp.float32)
    for block_index in range(N_RA):
        start = block_index * width
        piece = jnp.dot(stream[:, start:start + width], paired[start:start + width], preferred_element_type=jnp.float32)
        rounded = lax.optimization_barrier(piece.astype(jnp.bfloat16))
        total = total + rounded.astype(jnp.float32)
    return total

def sublayer(stream, w_gate, w_up, w_down, gain_row, shift_row):
    columns = w_gate.shape[1]
    paired = jnp.concatenate((w_gate, w_up), axis=1)
    summed = block_products(stream, paired)
    hidden = (jax.nn.silu(summed[:, :columns]) * summed[:, columns:]).astype(jnp.bfloat16)
    branch = jnp.dot(hidden, w_down, preferred_element_type=jnp.float32)
    mixed_rows = RESIDUAL * stream.astype(jnp.float32) + branch
    mean_rows = lax.optimization_barrier(jnp.sum(mixed_rows, axis=1)) / D
    var_rows = lax.optimization_barrier(jnp.sum(mixed_rows * mixed_rows, axis=1)) / D - mean_rows * mean_rows
    normed = (mixed_rows - mean_rows[:, None]) * lax.rsqrt(var_rows + EPSILON)[:, None]
    return (normed * gain_row + shift_row).astype(jnp.bfloat16)

def reference(inputs, gate_weight, up_weight, down_weight, norm_gain, norm_shift):
    stream = inputs
    for layer_index in range(LAYERS):
        stream = sublayer(stream, gate_weight[layer_index], up_weight[layer_index], down_weight[layer_index], norm_gain[layer_index], norm_shift[layer_index])
    return stream
```

```python
import jax
import jax.numpy as jnp
from jax import lax
from jax.sharding import Mesh
from jax.sharding import PartitionSpec as P

RESIDUAL = 0.5
EPSILON = 1e-05
BF16 = jnp.bfloat16
F32 = jnp.float32


def exchange(parts, axes):
    return lax.all_to_all(parts, axes, 0, 0, tiled=True)


def share(block, axes, peers):
    return exchange(jnp.broadcast_to(block[None], (peers, *block.shape)), axes)


def swap_core(block):
    return lax.ppermute(block, "c", [(0, 1), (1, 0)])


def dot_nt(a, b):
    return lax.dot_general(a, b, (((1,), (1,)), ((), ())), preferred_element_type=F32)


def regroup_weights(gate, up, down):
    stacked = jnp.stack((gate.T, up.T, down))
    rows = stacked.shape[1] // 4
    parts = stacked.reshape(3, 4, rows, 256).transpose(1, 0, 2, 3)
    mine = exchange(parts, "x")
    mine = mine.transpose(1, 2, 0, 3).reshape(3, rows, 1024)
    other = swap_core(mine)
    both = jnp.concatenate((mine, other), axis=1)
    return both[:2].reshape(2 * 2 * rows, 1024), both[2]


def normed(mixed, row_sum, row_squares, gain, shift):
    mean = row_sum / 4096.0
    var = row_squares / 4096.0 - mean * mean
    out = (mixed - mean[:, None]) * lax.rsqrt(var + EPSILON)[:, None]
    return (out * gain + shift).astype(BF16)


def hidden_units(stream, w_gu):
    partial = dot_nt(stream, w_gu).astype(BF16)
    cols = partial.shape[1] // 2
    summed = exchange(partial.reshape(4, -1, 2 * cols), "z").astype(F32).sum(axis=0)
    hidden = (jax.nn.silu(summed[:, :cols]) * summed[:, cols:]).astype(BF16)
    return share(hidden, "z", 4).reshape(-1, cols)


def per_device(inputs, gate_weight, up_weight, down_weight, norm_gain, norm_shift):
    c = lax.axis_index("c")
    x = lax.axis_index("x")
    y = lax.axis_index("y")
    half = inputs.shape[0] // 2
    quarter = half // 4
    mine = lax.dynamic_slice_in_dim(inputs, c * half + y * quarter, quarter, 0)
    rows = share(mine, "x", 4).transpose(1, 0, 2).reshape(quarter, 1024)
    stream = share(rows, "y", 4).reshape(half, 1024)
    affine = jnp.stack((norm_gain[0], norm_shift[0]))
    affine = lax.all_gather(affine, "x", axis=1, tiled=True)
    gu0, down0 = regroup_weights(gate_weight[0], up_weight[0], down_weight[0])
    gu1, down1 = regroup_weights(gate_weight[1], up_weight[1], down_weight[1])

    hidden = hidden_units(stream, gu0)
    partial = jnp.dot(hidden, down0, preferred_element_type=F32).astype(BF16)
    block = half // 16
    branch = exchange(partial.reshape(16, block, 1024), ("x", "y")).astype(F32).sum(axis=0)
    own = lax.dynamic_slice_in_dim(stream, (x * 4 + y) * block, block, 0)
    mixed = RESIDUAL * own.astype(F32) + branch
    stats = lax.psum(jnp.stack((mixed.sum(axis=1), (mixed * mixed).sum(axis=1))), "z")
    out = normed(mixed, stats[0], stats[1], affine[0], affine[1])
    stream = share(out, ("x", "y"), 16).reshape(half, 1024)

    hidden = hidden_units(stream, gu1)
    partial = jnp.dot(hidden, down1, preferred_element_type=F32).astype(BF16)
    parts = partial.reshape(4, quarter, 4, 256).transpose(2, 0, 1, 3).reshape(16, quarter, 256)
    branch = exchange(parts, ("x", "y")).astype(F32).sum(axis=0)
    own = lax.dynamic_slice(stream, (y * quarter, x * 256), (quarter, 256))
    mixed = RESIDUAL * own.astype(F32) + branch
    stats = lax.psum(jnp.stack((mixed.sum(axis=1), (mixed * mixed).sum(axis=1))), ("z", "x"))
    out = normed(mixed, stats[0], stats[1], norm_gain[1], norm_shift[1])
    ours = share(out, "y", 4).reshape(half, 256)
    theirs = swap_core(ours)
    result = jnp.concatenate((ours, theirs), axis=0)
    swapped = jnp.concatenate((theirs, ours), axis=0)
    return jnp.where(c == 0, result, swapped)


def solution(mesh):
    finer = Mesh(mesh.devices.reshape(4, 4, 4, 2), ("z", "x", "y", "c"))
    ra, cb = ("z", "x"), ("y", "c")
    in_specs = (
        P(None, ra),
        P(None, ra, cb),
        P(None, ra, cb),
        P(None, cb, ra),
        P(None, ra),
        P(None, ra),
    )
    return jax.shard_map(
        per_device, mesh=finer, in_specs=in_specs, out_specs=P(None, ra), check_vma=False
    )
```

```python
import functools

import jax
import jax.numpy as jnp
from jax import lax
from jax.experimental import pallas as pl
from jax.experimental.pallas import tpu as pltpu
from jax.sharding import Mesh
from jax.sharding import PartitionSpec as P

RESIDUAL = 0.5
EPSILON = 1e-05
WIDTH = 4096.0
BF16 = jnp.bfloat16
F32 = jnp.float32
ANY = pl.BlockSpec(memory_space=pl.ANY)
SMEM = pl.BlockSpec(memory_space=pltpu.SMEM)
VMEM = pl.BlockSpec(memory_space=pltpu.VMEM)


def exchange(parts, axes):
    return lax.all_to_all(parts, axes, 0, 0, tiled=True)


def share(block, axes, peers):
    return exchange(jnp.broadcast_to(block[None], (peers, *block.shape)), axes)


def shift(block, axis, step):
    return lax.ppermute(block, axis, [(i, (i + step) % 4) for i in range(4)])


def swap_core(block):
    return lax.ppermute(block, "c", [(0, 1), (1, 0)])


def share4(block, axis):
    return [block] + [shift(block, axis, step) for step in (1, 2, 3)]


def exchange4(parts, axis):
    return [parts[0]] + [shift(parts[step], axis, step) for step in (1, 2, 3)]


def behind(own, k):
    return lax.rem(own + 4 - k, 4)


def dot_nt(a, b):
    return lax.dot_general(a, b, (((1,), (1,)), ((), ())), preferred_element_type=F32)


def sds(*shape):
    return jax.ShapeDtypeStruct(shape, BF16)


def run_copies(copies, sems):
    started = []
    for i, (src, dst) in enumerate(copies):
        copy = pltpu.make_async_copy(src, dst, sems.at[i])
        copy.start()
        started.append(copy)
    return started


def pack_kernel(own_at, split, place_ref, gate_ref, up_ref, down_ref, *rest):
    outs, turned = rest[:-1], rest[-1]
    own = place_ref[own_at]
    cols = gate_ref.shape[2]
    for g, ref in enumerate((gate_ref, up_ref)):
        for at in range(0, cols, 128):
            turned[g, at : at + 128, :] = ref[0, :, at : at + 128].T
    rows = cols // 4
    for k in range(4):
        at = pl.ds(pl.multiple_of(lax.rem(own + k, 4) * rows, 16), rows)
        outs[k][0:2] = turned[:, at, :]
        if split:
            outs[4 + k][...] = down_ref[0, at, :]
        else:
            outs[k][2] = down_ref[0, at, :]


def pack(place, own_at, split, layer, gate, up, down):
    rows = gate.shape[2] // 4
    if split:
        out_shape = [sds(2, rows, 256)] * 4 + [sds(rows, 256)] * 4
    else:
        out_shape = [sds(3, rows, 256)] * 4
    pick = lambda i: (layer, 0, 0)
    return pl.pallas_call(
        functools.partial(pack_kernel, own_at, split),
        out_shape=out_shape,
        in_specs=[
            SMEM,
            pl.BlockSpec((1, *gate.shape[1:]), pick),
            pl.BlockSpec((1, *up.shape[1:]), pick),
            pl.BlockSpec((1, *down.shape[1:]), pick),
        ],
        out_specs=[VMEM] * len(out_shape),
        grid=(1,),
        scratch_shapes=[pltpu.VMEM((2, gate.shape[2], 256), BF16)],
    )(place, gate, up, down)


def gate_up_kernel(place_ref, *refs):
    rows, mine, theirs, outs = refs[:4], refs[4:8], refs[8:12], refs[12:16]
    stream, weights, sems = refs[16:]
    z, y = place_ref[0], place_ref[2]
    n, half = rows[0].shape[1], mine[0].shape[1]
    copies = []
    for m in range(4):
        lanes = slice(m * 256, m * 256 + 256)
        for s, piece in enumerate((mine[m], theirs[m])):
            for g in range(2):
                at = (2 * g + s) * half
                copies.append((piece.at[g], weights.at[at : at + half, lanes]))
    for j in range(4):
        for m in range(4):
            copies.append((rows[j].at[m], stream.at[behind(y, j), :, m * 256 : m * 256 + 256]))
    for copy in run_copies(copies, sems):
        copy.wait()
    for k in range(4):
        outs[k][...] = dot_nt(stream[lax.rem(z + k, 4)], weights[...]).astype(BF16)


def gate_up(place, rows, mine, theirs):
    n, half = rows[0].shape[1], mine[0].shape[1]
    return pl.pallas_call(
        gate_up_kernel,
        out_shape=[sds(n, 4 * half)] * 4,
        in_specs=[SMEM] + [ANY] * 12,
        out_specs=[VMEM] * 4,
        scratch_shapes=[
            pltpu.VMEM((4, n, 1024), BF16),
            pltpu.VMEM((4 * half, 1024), BF16),
            pltpu.SemaphoreType.DMA((32,)),
        ],
    )(place, *rows, *mine, *theirs)


def down_kernel(place_ref, *refs):
    hidden, mine, theirs, out = refs[:4], refs[4:8], refs[8:12], refs[12]
    rows, weights, sems = refs[13:]
    z, x = place_ref[0], place_ref[1]
    half = mine[0].shape[0]
    copies = []
    for m in range(4):
        lanes = pl.ds(pl.multiple_of(behind(x, m) * 256, 256), 256)
        copies.append((mine[m], weights.at[:half, lanes]))
        copies.append((theirs[m], weights.at[half:, lanes]))
    for k in range(4):
        copies.append((hidden[k], rows.at[behind(z, k)]))
    for copy in run_copies(copies, sems):
        copy.wait()
    n = rows.shape[1]
    for b in range(4):
        out[b * n : b * n + n, :] = jnp.dot(rows[b], weights[...], preferred_element_type=F32).astype(BF16)


def down(place, hidden, mine, theirs):
    n, cols = hidden[0].shape
    return pl.pallas_call(
        down_kernel,
        out_shape=sds(4 * n, 1024),
        in_specs=[SMEM] + [ANY] * 12,
        out_specs=VMEM,
        scratch_shapes=[
            pltpu.VMEM((4, n, cols), BF16),
            pltpu.VMEM((cols, 1024), BF16),
            pltpu.SemaphoreType.DMA((12,)),
        ],
    )(place, *hidden, *mine, *theirs)


def regroup_kernel(place_ref, *refs):
    pieces, outs, sems = refs[:4], refs[4:8], refs[8]
    x = place_ref[1]
    rows = outs[0].shape[2]
    copies = []
    for m in range(4):
        at = pl.ds(pl.multiple_of(lax.rem(x + m, 4) * rows, 8), rows)
        for k in range(4):
            copies.append((pieces[k].at[:, at, :], outs[m].at[k]))
    for copy in run_copies(copies, sems):
        copy.wait()


def regroup(place, pieces):
    rows = pieces[0].shape[1] // 4
    return pl.pallas_call(
        regroup_kernel,
        out_shape=[sds(4, 3, rows, 256)] * 4,
        in_specs=[SMEM] + [ANY] * 4,
        out_specs=[ANY] * 4,
        scratch_shapes=[pltpu.SemaphoreType.DMA((16,))],
    )(place, *pieces)


def join_kernel(*refs):
    pieces, outs, sems = refs[:4], refs[4:6], refs[6]
    copies = [(pieces[m], outs[m // 2].at[m % 2]) for m in range(4)]
    for copy in run_copies(copies, sems):
        copy.wait()


def join(pieces):
    return pl.pallas_call(
        join_kernel,
        out_shape=[sds(2, *pieces[0].shape)] * 2,
        in_specs=[ANY] * 4,
        out_specs=[ANY] * 2,
        scratch_shapes=[pltpu.SemaphoreType.DMA((4,))],
    )(*pieces)


def block_kernel(place_ref, rows_ref, *refs):
    pieces, out, own_out = refs[:16], refs[16], refs[17]
    stream, w_gu, w_down, row_sems, sems = refs[18:]
    z, x = place_ref[0], place_ref[1]
    n = rows_ref.shape[1]
    cols = pieces[0].shape[3]
    copies = []
    for i in range(16):
        copies.append((rows_ref.at[i], stream.at[i % 4 * n : i % 4 * n + n, i // 4 * 1024 : i // 4 * 1024 + 1024]))
    row_copies = run_copies(copies, row_sems)
    copies = []
    for p in range(8):
        for h in range(2):
            piece = pieces[2 * p + h]
            for m in range(2):
                for g in range(2):
                    copies.append((piece.at[m, :, g], w_gu.at[2 * h + m, :, g, p]))
    for p in range(8):
        for h in range(2):
            piece = pieces[2 * p + h]
            for m in range(2):
                copies.append((piece.at[m, :, 2], w_down.at[2 * h + m, :, p]))
    weight_copies = run_copies(copies, sems)
    for copy in row_copies:
        copy.wait()
    for copy in weight_copies[:64]:
        copy.wait()
    total = [None, None]
    for m in range(4):
        for k in range(4):
            at = behind(z, k) * 4 + behind(x, m)
            block = stream[:, pl.ds(pl.multiple_of(at * 256, 256), 256)]
            if m == 0 and k == 0:
                own_out[...] = block
            for g in range(2):
                part = dot_nt(block, w_gu[m, k, g].reshape(8 * cols, 256))
                total[g] = part if total[g] is None else total[g] + part
    hidden = (total[0] * jax.nn.sigmoid(total[0]) * total[1]).astype(BF16)
    for copy in weight_copies[64:]:
        copy.wait()
    for m in range(4):
        for k in range(4):
            at = behind(z, k) * 4 + behind(x, m)
            part = jnp.dot(hidden, w_down[m, k].reshape(8 * cols, 256), preferred_element_type=F32)
            out[at] = part.astype(BF16)


def block_layer(place, rows, pieces):
    n = rows.shape[1]
    cols = pieces[0].shape[3]
    return pl.pallas_call(
        block_kernel,
        out_shape=[sds(16, 4 * n, 256), sds(4 * n, 256)],
        in_specs=[SMEM] + [ANY] * 17,
        out_specs=[VMEM] * 2,
        scratch_shapes=[
            pltpu.VMEM((4 * n, 4096), BF16),
            pltpu.VMEM((4, 4, 2, 8, cols, 256), BF16),
            pltpu.VMEM((4, 4, 8, cols, 256), BF16),
            pltpu.SemaphoreType.DMA((16,)),
            pltpu.SemaphoreType.DMA((96,)),
        ],
    )(place, rows, *pieces)


def normed(mixed, row_sum, row_squares, gain, shift_row):
    mean = row_sum / WIDTH
    var = row_squares / WIDTH - mean * mean
    out = (mixed - mean[:, None]) * lax.rsqrt(var + EPSILON)[:, None]
    return (out * gain + shift_row).astype(BF16)


def row_stats(mixed):
    return jnp.stack((mixed.sum(axis=1), (mixed * mixed).sum(axis=1)))


def in_order(pieces, own):
    back = [pieces[0], pieces[3], pieces[2], pieces[1]]
    twice = jnp.stack(back + back[:3])
    return lax.dynamic_slice_in_dim(twice, (4 - own) % 4, 4, 0)


def per_device(inputs, gate_weight, up_weight, down_weight, norm_gain, norm_shift):
    z, x, y, c = (lax.axis_index(a) for a in ("z", "x", "y", "c"))
    place = jnp.stack((z, x, y, c)).astype(jnp.int32)
    half = inputs.shape[0] // 2
    quarter = half // 4
    block = half // 16
    cols = gate_weight.shape[2] // 2

    with jax.named_scope("rows_in"):
        mine = lax.dynamic_slice_in_dim(inputs, c * half + y * quarter, quarter, 0)
        rows = share4(jnp.stack(share4(mine, "x")), "y")

    with jax.named_scope("w0"):
        packed = pack(place, 1, True, 0, gate_weight, up_weight, down_weight)
        gu0 = exchange4(packed[:4], "x")
        gu0_core = [swap_core(w) for w in gu0]
        down0 = exchange4(packed[4:], "x")
        down0_core = [swap_core(w) for w in down0]

    with jax.named_scope("affine"):
        affine = in_order(share4(jnp.stack((norm_gain[0], norm_shift[0])), "x"), x)
        affine = affine.transpose(1, 0, 2).reshape(2, 1024)

    with jax.named_scope("w1"):
        packed = pack(place, 0, False, 1, gate_weight, up_weight, down_weight)
        pieces = exchange4(regroup(place, exchange4(packed, "z")), "x")
        first, second = join(pieces)
        near = [shift(first, "y", 1), shift(second, "y", 1)]
        far = [shift(first, "y", 3), shift(second, "y", 3)]
        across = [shift(near[0], "y", 1), shift(far[1], "y", 3)]
        w1 = [first, second, *near, *across, *far]
        w1 = w1 + [swap_core(w) for w in w1]

    with jax.named_scope("layer0"):
        sums = exchange4(gate_up(place, rows, gu0, gu0_core), "z")
        summed = sum(piece.astype(F32) for piece in sums)
        hidden = (jax.nn.silu(summed[:, :cols]) * summed[:, cols:]).astype(BF16)
        partial = down(place, share4(hidden, "z"), down0, down0_core)
        branch = exchange(partial.reshape(16, block, 1024), ("y", "x")).astype(F32).sum(axis=0)
        own = lax.dynamic_slice_in_dim(rows[0], x * block, block, 1)
        own = in_order([own[m] for m in range(4)], x).transpose(1, 0, 2).reshape(block, 1024)
        mixed = RESIDUAL * own.astype(F32) + branch
        stats = share(row_stats(mixed), "z", 4).sum(axis=0)
        out = normed(mixed, stats[0], stats[1], affine[0], affine[1])
        stream = share(out, ("z", "x"), 16)

    with jax.named_scope("layer1"):
        parts, own = block_layer(place, stream, w1)
        branch = exchange(parts, ("z", "x")).astype(F32).sum(axis=0)
        mixed = RESIDUAL * own.astype(F32) + branch
        stats = share(row_stats(mixed), ("z", "x"), 16).sum(axis=0)
        out = normed(mixed, stats[0], stats[1], norm_gain[1], norm_shift[1])

    with jax.named_scope("rows_out"):
        ours = share(out, "y", 4).reshape(half, 256)
        theirs = swap_core(ours)
        return jnp.where(c == 0, jnp.concatenate((ours, theirs)), jnp.concatenate((theirs, ours)))


def solution(mesh):
    finer = Mesh(mesh.devices.reshape(4, 4, 4, 2), ("z", "x", "y", "c"))
    ra, cb = ("z", "x"), ("y", "c")
    in_specs = (
        P(None, ra),
        P(None, ra, cb),
        P(None, ra, cb),
        P(None, cb, ra),
        P(None, ra),
        P(None, ra),
    )
    return jax.shard_map(
        per_device, mesh=finer, in_specs=in_specs, out_specs=P(None, ra), check_vma=False
    )
```

```python
import jax
import jax.numpy as jnp
from jax import lax
from jax.experimental import pallas as pl
from jax.experimental.pallas import tpu as pltpu
from jax.sharding import Mesh
from jax.sharding import PartitionSpec as P

RESIDUAL = 0.5
EPSILON = 1e-05
WIDTH = 4096.0
BF16 = jnp.bfloat16
F32 = jnp.float32
ANY = pl.BlockSpec(memory_space=pl.ANY)
SMEM = pl.BlockSpec(memory_space=pltpu.SMEM)
VMEM = pl.BlockSpec(memory_space=pltpu.VMEM)


def exchange(parts, axes):
    return lax.all_to_all(parts, axes, 0, 0, tiled=True)


def share(block, axes, peers):
    return exchange(jnp.broadcast_to(block[None], (peers, *block.shape)), axes)


def shift(block, axis, step):
    return lax.ppermute(block, axis, [(i, (i + step) % 4) for i in range(4)])


def swap_core(block):
    return lax.ppermute(block, "c", [(0, 1), (1, 0)])


def share4(block, axis):
    return exchange4([block] * 4, axis)


def exchange4(parts, axis):
    got = [parts[0]]
    for step in (1, 2, 3):
        got.append(shift(parts[step], axis, step))
    return got


def behind(own, k):
    return lax.rem(own + 4 - k, 4)


def dot_nt(a, b):
    return lax.dot_general(a, b, (((1,), (1,)), ((), ())), preferred_element_type=F32)


def sds(*shape):
    return jax.ShapeDtypeStruct(shape, BF16)


def run_copies(copies, sems):
    started = []
    for i, (src, dst) in enumerate(copies):
        copy = pltpu.make_async_copy(src, dst, sems.at[i])
        copy.start()
        started.append(copy)
    return started


def turn_kernel(gate_ref, up_ref, down_ref, out):
    rows = out.shape[2]
    for g, ref in enumerate((gate_ref, up_ref)):
        turned = ref[0].T
        for p in range(16):
            out[p, g] = turned[p * rows : p * rows + rows]
    for p in range(16):
        out[p, 2] = down_ref[0, p * rows : p * rows + rows]


def turn(layer, gate, up, down):
    rows = gate.shape[2] // 16
    pick = lambda i: (layer, 0, 0)
    return pl.pallas_call(
        turn_kernel,
        out_shape=sds(16, 3, rows, 256),
        in_specs=[
            pl.BlockSpec((1, *gate.shape[1:]), pick),
            pl.BlockSpec((1, *up.shape[1:]), pick),
            pl.BlockSpec((1, *down.shape[1:]), pick),
        ],
        out_specs=VMEM,
        grid=(1,),
    )(gate, up, down)


def pack_kernel(place_ref, gate_ref, up_ref, down_ref, *rest):
    outs, turned = rest[:-1], rest[-1]
    own = place_ref[1]
    cols = gate_ref.shape[2]
    for g, ref in enumerate((gate_ref, up_ref)):
        for at in range(0, cols, 128):
            turned[g, at : at + 128, :] = ref[0, :, at : at + 128].T
    rows = cols // 4
    for k in range(4):
        at = pl.ds(pl.multiple_of(lax.rem(own + k, 4) * rows, 16), rows)
        outs[k][0:2] = turned[:, at, :]
        outs[4 + k][...] = down_ref[0, at, :]


def pack(place, layer, gate, up, down):
    rows = gate.shape[2] // 4
    out_shape = [sds(2, rows, 256)] * 4 + [sds(rows, 256)] * 4
    pick = lambda i: (layer, 0, 0)
    return pl.pallas_call(
        pack_kernel,
        out_shape=out_shape,
        in_specs=[
            SMEM,
            pl.BlockSpec((1, *gate.shape[1:]), pick),
            pl.BlockSpec((1, *up.shape[1:]), pick),
            pl.BlockSpec((1, *down.shape[1:]), pick),
        ],
        out_specs=[VMEM] * len(out_shape),
        grid=(1,),
        scratch_shapes=[pltpu.VMEM((2, gate.shape[2], 256), BF16)],
    )(place, gate, up, down)


def gate_up_kernel(place_ref, *refs):
    rows, mine, theirs, outs = refs[:4], refs[4:8], refs[8:12], refs[12:16]
    stream, weights, sems = refs[16:]
    z, y = place_ref[0], place_ref[2]
    half = mine[0].shape[1]
    copies = []
    for m in range(4):
        lanes = slice(m * 256, m * 256 + 256)
        for s, piece in enumerate((mine[m], theirs[m])):
            for g in range(2):
                at = (2 * g + s) * half
                copies.append((piece.at[g], weights.at[at : at + half, lanes]))
    for j in range(4):
        for m in range(4):
            copies.append((rows[j].at[m], stream.at[behind(y, j), :, m * 256 : m * 256 + 256]))
    for copy in run_copies(copies, sems):
        copy.wait()
    for k in range(4):
        outs[k][...] = dot_nt(stream[lax.rem(z + k, 4)], weights[...]).astype(BF16)


def gate_up(place, rows, mine, theirs):
    n, half = rows[0].shape[1], mine[0].shape[1]
    return pl.pallas_call(
        gate_up_kernel,
        out_shape=[sds(n, 4 * half)] * 4,
        in_specs=[SMEM] + [ANY] * 12,
        out_specs=[VMEM] * 4,
        scratch_shapes=[
            pltpu.VMEM((4, n, 1024), BF16),
            pltpu.VMEM((4 * half, 1024), BF16),
            pltpu.SemaphoreType.DMA((32,)),
        ],
    )(place, *rows, *mine, *theirs)


def down_kernel(place_ref, *refs):
    hidden, mine, theirs, out = refs[:4], refs[4:8], refs[8:12], refs[12]
    rows, weights, sems = refs[13:]
    z, x = place_ref[0], place_ref[1]
    half = mine[0].shape[0]
    copies = []
    for m in range(4):
        lanes = pl.ds(pl.multiple_of(behind(x, m) * 256, 256), 256)
        copies.append((mine[m], weights.at[:half, lanes]))
        copies.append((theirs[m], weights.at[half:, lanes]))
    for k in range(4):
        copies.append((hidden[k], rows.at[behind(z, k)]))
    for copy in run_copies(copies, sems):
        copy.wait()
    n = rows.shape[1]
    for b in range(4):
        out[b * n : b * n + n, :] = jnp.dot(rows[b], weights[...], preferred_element_type=F32).astype(BF16)


def down(place, hidden, mine, theirs):
    n, cols = hidden[0].shape
    return pl.pallas_call(
        down_kernel,
        out_shape=sds(4 * n, 1024),
        in_specs=[SMEM] + [ANY] * 12,
        out_specs=VMEM,
        scratch_shapes=[
            pltpu.VMEM((4, n, cols), BF16),
            pltpu.VMEM((cols, 1024), BF16),
            pltpu.SemaphoreType.DMA((12,)),
        ],
    )(place, *hidden, *mine, *theirs)


def block_kernel(place_ref, rows_ref, *refs):
    pieces, out, own_out = refs[:10], refs[10], refs[11]
    stream, w_gu, w_down, row_sems, sems = refs[12:]
    z, x = place_ref[0], place_ref[1]
    n = rows_ref.shape[1]
    cols = pieces[0].shape[3]
    copies = []
    for i in range(16):
        copies.append((rows_ref.at[i], stream.at[i % 4 * n : i % 4 * n + n, i // 4 * 1024 : i // 4 * 1024 + 1024]))
    row_copies = run_copies(copies, row_sems)
    spans = [(q, slice(0, 4)) for q in range(3)] + [(3, slice(0, 2)), (3, slice(2, 4))]
    copies = []
    for i, piece in enumerate(pieces):
        slot, span = spans[i % 5]
        for g in range(2):
            copies.append((piece.at[:, :, g], w_gu.at[span, :, g, slot + 4 * (i // 5)]))
    for i, piece in enumerate(pieces):
        slot, span = spans[i % 5]
        copies.append((piece.at[:, :, 2], w_down.at[span, :, slot + 4 * (i // 5)]))
    weight_copies = run_copies(copies, sems)
    for copy in row_copies:
        copy.wait()
    for copy in weight_copies[:20]:
        copy.wait()
    at = z * 4 + x
    own_out[...] = stream[:, pl.ds(pl.multiple_of(at * 256, 256), 256)]
    total = [None, None]
    for i in range(16):
        block = stream[:, i * 256 : i * 256 + 256]
        for g in range(2):
            part = dot_nt(block, w_gu[i // 4, i % 4, g].reshape(8 * cols, 256))
            total[g] = part if total[g] is None else total[g] + part
    hidden = (total[0] * jax.nn.sigmoid(total[0]) * total[1]).astype(BF16)
    for copy in weight_copies[20:]:
        copy.wait()
    for i in range(16):
        part = jnp.dot(hidden, w_down[i // 4, i % 4].reshape(8 * cols, 256), preferred_element_type=F32)
        out[i] = part.astype(BF16)


def block_layer(place, rows, pieces):
    n = rows.shape[1]
    cols = pieces[0].shape[3]
    return pl.pallas_call(
        block_kernel,
        out_shape=[sds(16, 4 * n, 256), sds(4 * n, 256)],
        in_specs=[SMEM] + [ANY] * 11,
        out_specs=[VMEM] * 2,
        scratch_shapes=[
            pltpu.VMEM((4 * n, 4096), BF16),
            pltpu.VMEM((4, 4, 2, 8, cols, 256), BF16),
            pltpu.VMEM((4, 4, 8, cols, 256), BF16),
            pltpu.SemaphoreType.DMA((16,)),
            pltpu.SemaphoreType.DMA((30,)),
        ],
    )(place, rows, *pieces)


def normed(mixed, row_sum, row_squares, gain, shift_row):
    mean = row_sum / WIDTH
    var = row_squares / WIDTH - mean * mean
    out = (mixed - mean[:, None]) * lax.rsqrt(var + EPSILON)[:, None]
    return (out * gain + shift_row).astype(BF16)


def row_stats(mixed):
    return jnp.stack((mixed.sum(axis=1), (mixed * mixed).sum(axis=1)))


def in_order(pieces, own):
    back = jnp.concatenate((pieces[:1], pieces[3:4], pieces[2:3], pieces[1:2]))
    return lax.dynamic_slice_in_dim(jnp.concatenate((back, back[:3])), (4 - own) % 4, 4, 0)


def thirds(values):
    high = lax.reduce_precision(values, 8, 7)
    middle = lax.reduce_precision(values - high, 8, 7)
    low = values - high - middle
    return jnp.concatenate((high, middle, low)).astype(BF16)


def per_device(inputs, gate_weight, up_weight, down_weight, norm_gain, norm_shift):
    z, x, y, c = (lax.axis_index(a) for a in ("z", "x", "y", "c"))
    place = jnp.stack((z, x, y, c)).astype(jnp.int32)
    half = inputs.shape[0] // 2
    quarter = half // 4
    block = half // 16
    cols = gate_weight.shape[2] // 2

    mine = lax.dynamic_slice_in_dim(inputs, c * half + y * quarter, quarter, 0)
    affine = thirds(jnp.stack((norm_gain[0], norm_shift[0])))
    mine = jnp.concatenate((mine, affine, jnp.zeros((2, 256), BF16)))
    mine = jnp.stack(share4(mine, "x"))
    rows = share4(mine[:, :quarter], "y")

    packed = pack(place, 0, gate_weight, up_weight, down_weight)
    gu0 = exchange4(packed[:4], "x")
    down0 = exchange4(packed[4:], "x")
    gu0_core = [swap_core(w) for w in gu0]
    down0_core = [swap_core(w) for w in down0]

    w1 = turn(1, gate_weight, up_weight, down_weight)
    w1 = exchange(w1, ("z", "x")).reshape(4, 4, *w1.shape[1:])
    near = shift(w1, "y", 1)
    far = shift(w1, "y", 3)
    across = [shift(near[:2], "y", 1)]
    across.append(shift(far[2:], "y", 3))
    w1 = [w1, near, far, *across]
    w1_core = []
    for w in w1:
        w1_core.append(swap_core(w))

    sums = gate_up(place, rows, gu0, gu0_core)
    sums = exchange4(sums, "z")
    summed = sum(piece.astype(F32) for piece in sums)
    hidden = (jax.nn.silu(summed[:, :cols]) * summed[:, cols:]).astype(BF16)
    hidden = share4(hidden, "z")
    partial = down(place, hidden, down0, down0_core)
    branch = exchange(partial.reshape(16, block, 1024), ("y", "x"))
    branch = branch.astype(F32).sum(axis=0)
    own = lax.dynamic_slice_in_dim(rows[0], x * block, block, 1)
    own = in_order(own, x).transpose(1, 0, 2).reshape(block, 1024)
    affine = in_order(mine[:, quarter : quarter + 6].astype(F32), x)
    affine = (affine[:, :2] + affine[:, 2:4]) + affine[:, 4:]
    affine = affine.transpose(1, 0, 2).reshape(2, 1024)
    mixed = RESIDUAL * own.astype(F32) + branch
    stats = share(row_stats(mixed), "z", 4).sum(axis=0)
    out = normed(mixed, stats[0], stats[1], affine[0], affine[1])
    stream = share(out, ("z", "x"), 16)

    parts, own = block_layer(place, stream, w1 + w1_core)
    branch = exchange(parts, ("z", "x")).astype(F32).sum(axis=0)
    mixed = RESIDUAL * own.astype(F32) + branch
    stats = share(row_stats(mixed), ("z", "x"), 16).sum(axis=0)
    out = normed(mixed, stats[0], stats[1], norm_gain[1], norm_shift[1])
    ours = share(out, "y", 4).reshape(half, 256)
    theirs = swap_core(ours)
    return jnp.where(c == 0, jnp.concatenate((ours, theirs)), jnp.concatenate((theirs, ours)))


def solution(mesh):
    finer = Mesh(mesh.devices.reshape(4, 4, 4, 2), ("z", "x", "y", "c"))
    ra, cb = ("z", "x"), ("y", "c")
    in_specs = (
        P(None, ra),
        P(None, ra, cb),
        P(None, ra, cb),
        P(None, cb, ra),
        P(None, ra),
        P(None, ra),
    )


    return jax.shard_map(
        per_device, mesh=finer, in_specs=in_specs, out_specs=P(None, ra), check_vma=False
    )
```

```python
import jax
import jax.numpy as jnp
from jax import lax
from jax.experimental import pallas as pl
from jax.experimental.pallas import tpu as pltpu
from jax.sharding import Mesh
from jax.sharding import PartitionSpec as P

RESIDUAL = 0.5
EPSILON = 1e-05
WIDTH = 4096.0
BF16 = jnp.bfloat16
F32 = jnp.float32
ANY = pl.BlockSpec(memory_space=pltpu.HBM)
SMEM = pl.BlockSpec(memory_space=pltpu.SMEM)
VMEM = pl.BlockSpec(memory_space=pltpu.VMEM)


def exchange(parts, axes):
    return lax.all_to_all(parts, axes, 0, 0, tiled=True)


def share(block, axes, peers):
    return exchange(jnp.broadcast_to(block[None], (peers, *block.shape)), axes)


def shift(block, axis, step):
    return lax.ppermute(block, axis, [(i, (i + step) % 4) for i in range(4)])


def in_vmem(value):
    return pltpu.with_memory_space_constraint(value, pltpu.VMEM)


def swap_core(block):
    return lax.ppermute(block, "c", [(0, 1), (1, 0)])


def share4(block, axis):
    return exchange4([block] * 4, axis)


def exchange4(parts, axis):
    got = [parts[0]]
    for step in (1, 2, 3):
        got.append(shift(parts[step], axis, step))
    return got


def behind(own, k):
    return lax.rem(own + 4 - k, 4)


def dot_nt(a, b):
    return lax.dot_general(a, b, (((1,), (1,)), ((), ())), preferred_element_type=F32)


def sds(*shape):
    return jax.ShapeDtypeStruct(shape, BF16)


def run_copies(copies, sems):
    started = []
    for i, (src, dst) in enumerate(copies):
        copy = pltpu.make_async_copy(src, dst, sems.at[i])
        copy.start()
        started.append(copy)
    return started


def turn_kernel(gate_ref, up_ref, down_ref, out):
    rows = out.shape[2]
    for g, ref in enumerate((gate_ref, up_ref)):
        turned = ref[0].T
        for p in range(4):
            out[p, g] = turned[p * rows : p * rows + rows]
    for p in range(4):
        out[p, 2] = down_ref[0, p * rows : p * rows + rows]


def turn(layer, gate, up, down):
    rows = gate.shape[2] // 4
    pick = lambda i: (layer, 0, 0)
    return pl.pallas_call(
        turn_kernel,
        out_shape=sds(4, 3, rows, 256),
        in_specs=[
            pl.BlockSpec((1, *gate.shape[1:]), pick),
            pl.BlockSpec((1, *up.shape[1:]), pick),
            pl.BlockSpec((1, *down.shape[1:]), pick),
        ],
        out_specs=VMEM,
        grid=(1,),
    )(gate, up, down)


def pack_kernel(place_ref, gate_ref, up_ref, down_ref, *rest):
    outs, turned = rest[:-1], rest[-1]
    own = place_ref[1]
    cols = gate_ref.shape[2]
    for g, ref in enumerate((gate_ref, up_ref)):
        for at in range(0, cols, 128):
            turned[g, at : at + 128, :] = ref[0, :, at : at + 128].T
    rows = cols // 4
    for k in range(4):
        at = pl.ds(pl.multiple_of(lax.rem(own + k, 4) * rows, 16), rows)
        outs[k][0:2] = turned[:, at, :]
        outs[4 + k][...] = down_ref[0, at, :]


def pack(place, layer, gate, up, down):
    rows = gate.shape[2] // 4
    out_shape = [sds(2, rows, 256)] * 4 + [sds(rows, 256)] * 4
    pick = lambda i: (layer, 0, 0)
    return pl.pallas_call(
        pack_kernel,
        out_shape=out_shape,
        in_specs=[
            SMEM,
            pl.BlockSpec((1, *gate.shape[1:]), pick),
            pl.BlockSpec((1, *up.shape[1:]), pick),
            pl.BlockSpec((1, *down.shape[1:]), pick),
        ],
        out_specs=[VMEM] * len(out_shape),
        grid=(1,),
        scratch_shapes=[pltpu.VMEM((2, gate.shape[2], 256), BF16)],
    )(place, gate, up, down)


def gate_up_kernel(place_ref, *refs):
    rows, mine, theirs, outs, own_out = refs[:4], refs[4:8], refs[8:12], refs[12:19], refs[19]
    stream, weights, partial, sems, out_sems = refs[20:]
    z, x, y = place_ref[0], place_ref[1], place_ref[2]
    n, half = rows[0].shape[1], mine[0].shape[1]
    block = own_out.shape[0]
    lanes = [pl.ds(pl.multiple_of(behind(x, m) * 256, 256), 256) for m in range(4)]
    copies = []
    for j in range(4):
        for m in range(4):
            copies.append((rows[j].at[m], stream.at[behind(y, j), :, lanes[m]]))
    for g in range(2):
        for m in range(4):
            for s, piece in enumerate((mine[m], theirs[m])):
                at = (2 * g + s) * half
                copies.append((piece.at[g], weights.at[at : at + half, lanes[m]]))
    started = run_copies(copies, sems)
    for copy in started[:24]:
        copy.wait()
    own_out[...] = stream[x, pl.ds(pl.multiple_of(y * block, 16), block), :]
    whole = stream[...].reshape(4 * n, 1024)
    for g in range(2):
        at = slice(2 * g * half, 2 * g * half + 2 * half)
        if g == 1:
            for copy in started[24:]:
                copy.wait()
        partial[:, :, at] = dot_nt(whole, weights[at]).astype(BF16).reshape(4, n, 2 * half)
    copies = [(partial.at[z], outs[0])]
    for k in range(1, 4):
        for h in range(2):
            src = partial.at[lax.rem(z + k, 4), h * n // 2 : h * n // 2 + n // 2]
            copies.append((src, outs[2 * k - 1 + h]))
    for copy in run_copies(copies, out_sems):
        copy.wait()


def gate_up(place, rows, mine, theirs):
    n, half = rows[0].shape[1], mine[0].shape[1]
    return pl.pallas_call(
        gate_up_kernel,
        out_shape=[sds(n, 4 * half)] + [sds(n // 2, 4 * half)] * 6 + [sds(n // 4, 1024)],
        in_specs=[SMEM] + [ANY] * 12,
        out_specs=[ANY] * 7 + [VMEM],
        scratch_shapes=[
            pltpu.VMEM((4, n, 1024), BF16),
            pltpu.VMEM((4 * half, 1024), BF16),
            pltpu.VMEM((4, n, 4 * half), BF16),
            pltpu.SemaphoreType.DMA((32,)),
            pltpu.SemaphoreType.DMA((7,)),
        ],
    )(place, *rows, *mine, *theirs)


def down_kernel(place_ref, *refs):
    hidden, mine, theirs, out = refs[:4], refs[4:8], refs[8:12], refs[12]
    rows, weights, sems = refs[13:]
    z, x = place_ref[0], place_ref[1]
    half = mine[0].shape[0]
    copies = []
    for m in range(4):
        lanes = pl.ds(pl.multiple_of(behind(x, m) * 256, 256), 256)
        copies.append((mine[m], weights.at[:half, lanes]))
        copies.append((theirs[m], weights.at[half:, lanes]))
    for k in range(4):
        copies.append((hidden[k], rows.at[behind(z, k)]))
    for copy in run_copies(copies, sems):
        copy.wait()
    n, cols = rows.shape[1:]
    out[...] = jnp.dot(rows[...].reshape(4 * n, cols), weights[...], preferred_element_type=F32).astype(BF16)


def down(place, hidden, mine, theirs):
    n, cols = hidden[0].shape
    return pl.pallas_call(
        down_kernel,
        out_shape=sds(4 * n, 1024),
        in_specs=[SMEM] + [ANY] * 12,
        out_specs=VMEM,
        scratch_shapes=[
            pltpu.VMEM((4, n, cols), BF16),
            pltpu.VMEM((cols, 1024), BF16),
            pltpu.SemaphoreType.DMA((12,)),
        ],
    )(place, *hidden, *mine, *theirs)


def parts_of(value):
    high = value.astype(BF16)
    rest = value - high.astype(F32)
    middle = rest.astype(BF16)
    return high, middle, (rest - middle.astype(F32)).astype(BF16)


def norm_kernel(branch, own, out, message, sems):
    mixed = RESIDUAL * own[...].astype(F32)
    for i in range(branch.shape[0]):
        mixed += branch[i].astype(F32)
    cols = mixed.shape[1]
    mean = mixed.sum(axis=1, keepdims=True) / cols
    mixed -= mean
    message[:, :cols] = mixed.astype(BF16)
    lane = lax.broadcasted_iota(jnp.int32, (mixed.shape[0], 128), 1)
    tail = jnp.zeros((mixed.shape[0], 128), F32)
    for i, part in enumerate(parts_of(mean) + parts_of((mixed * mixed).sum(axis=1, keepdims=True))):
        tail = jnp.where(lane == i, part.astype(F32), tail)
    message[:, cols:] = tail.astype(BF16)
    for copy in run_copies([(message, out.at[i]) for i in range(out.shape[0])], sems):
        copy.wait()


def norm_message(branch, own):
    n, cols = own.shape
    return pl.pallas_call(
        norm_kernel,
        out_shape=sds(16, n, cols + 128),
        in_specs=[VMEM] * 2,
        out_specs=ANY,
        scratch_shapes=[pltpu.VMEM((n, cols + 128), BF16), pltpu.SemaphoreType.DMA((16,))],
        compiler_params=pltpu.CompilerParams(vmem_limit_bytes=16 << 20),
    )(branch, own)


def block_kernel(place_ref, rows_ref, affine_ref, *refs):
    pieces, out, own_out = refs[:16], refs[16], refs[17]
    stream, tails, weights, row_sems, sems = refs[18:]
    z, x, y = place_ref[0], place_ref[1], place_ref[2]
    n, rows = rows_ref.shape[1], pieces[0].shape[2]
    copies = []
    for i in range(16):
        at = slice(i % 4 * n, i % 4 * n + n)
        copies.append((rows_ref.at[i, :, :1024], stream.at[at, i // 4 * 1024 : i // 4 * 1024 + 1024]))
        copies.append((rows_ref.at[i, :, 1024:], tails.at[i // 4, at]))
    row_copies = run_copies(copies, row_sems)

    def load(g):
        for i, piece in enumerate(pieces):
            at, step, first = i // 8 * rows, (0, 1, 3, 2)[i % 8 // 2], i % 2 * 2
            for q in range(2):
                lanes = pl.ds(pl.multiple_of((first + q) * 1024 + behind(x, step) * 256, 256), 256)
                pltpu.make_async_copy(piece.at[q, g], weights.at[g, at : at + rows, lanes], sems.at[g]).start()

    def loaded(g):
        pltpu.make_async_copy(weights.at[g], weights.at[g], sems.at[g]).wait()

    load(0)
    for copy in row_copies:
        copy.wait()
    means, squares = [], []
    for q in range(4):
        tail = tails[q].astype(F32)
        means.append(tail[:, 0:1] + tail[:, 1:2] + tail[:, 2:3])
        squares.append(tail[:, 3:4] + tail[:, 4:5] + tail[:, 5:6])
    mean = sum(means) / 4
    square = sum(squares) + sum((m - mean) * (m - mean) for m in means) * 1024
    scale = lax.rsqrt(square / WIDTH + EPSILON)
    for q in range(4):
        at = slice(q * 1024, q * 1024 + 1024)
        value = (stream[:, at].astype(F32) + (means[q] - mean)) * scale
        stream[:, at] = (value * affine_ref[0:1, at] + affine_ref[1:2, at]).astype(BF16)
    own_out[...] = stream[pl.ds(pl.multiple_of(y * n, 16), n), pl.ds(pl.multiple_of(z * 1024, 1024), 1024)]
    loaded(0)
    load(1)
    load(2)
    gate = dot_nt(stream[...], weights[0])
    gate = gate * jax.nn.sigmoid(gate)
    loaded(1)
    hidden = (gate * dot_nt(stream[...], weights[1])).astype(BF16)
    loaded(2)
    for q in range(4):
        part = jnp.dot(hidden, weights[2, :, q * 1024 : q * 1024 + 1024], preferred_element_type=F32)
        out[4 * q : 4 * q + 4] = part.astype(BF16).reshape(4, n, 1024)


def block_layer(place, rows, affine, pieces):
    n, half = rows.shape[1], pieces[0].shape[2]
    return pl.pallas_call(
        block_kernel,
        out_shape=[sds(16, n, 1024), sds(n, 1024)],
        in_specs=[SMEM, VMEM, VMEM] + [ANY] * 16,
        out_specs=[VMEM] * 2,
        scratch_shapes=[
            pltpu.VMEM((4 * n, 4096), BF16),
            pltpu.VMEM((4, 4 * n, 128), BF16),
            pltpu.VMEM((3, 2 * half, 4096), BF16),
            pltpu.SemaphoreType.DMA((32,)),
            pltpu.SemaphoreType.DMA((3,)),
        ],
        compiler_params=pltpu.CompilerParams(vmem_limit_bytes=40 << 20),
    )(place, rows, affine, *pieces)


def normed(mixed, row_sum, row_squares, gain, shift_row):
    mean = row_sum / WIDTH
    var = row_squares / WIDTH - mean * mean
    out = (mixed - mean[:, None]) * lax.rsqrt(var + EPSILON)[:, None]
    return (out * gain + shift_row).astype(BF16)


def row_stats(mixed):
    return jnp.stack((mixed.sum(axis=1), (mixed * mixed).sum(axis=1)))


def in_order(pieces, own):
    back = jnp.concatenate((pieces[:1], pieces[3:4], pieces[2:3], pieces[1:2]))
    return lax.dynamic_slice_in_dim(jnp.concatenate((back, back[:3])), (4 - own) % 4, 4, 0)


def thirds(values):
    high = lax.reduce_precision(values, 8, 7)
    middle = lax.reduce_precision(values - high, 8, 7)
    low = values - high - middle
    return jnp.concatenate((high, middle, low)).astype(BF16)


def per_device(inputs, gate_weight, up_weight, down_weight, norm_gain, norm_shift):
    z, x, y, c = (lax.axis_index(a) for a in ("z", "x", "y", "c"))
    place = jnp.stack((z, x, y, c)).astype(jnp.int32)
    half = inputs.shape[0] // 2
    quarter = half // 4
    block = half // 16
    cols = gate_weight.shape[2] // 2

    mine = lax.dynamic_slice_in_dim(inputs, c * half + y * quarter, quarter, 0)
    affine = thirds(jnp.concatenate((norm_gain, norm_shift)))
    mine = jnp.concatenate((mine, affine, jnp.zeros((4, 256), BF16)))
    mine = jnp.stack(share4(mine, "x"))
    rows = share4(mine[:, :quarter], "y")

    packed = pack(place, 0, gate_weight, up_weight, down_weight)
    gu0 = exchange4(packed[:4], "x")
    down0 = exchange4(packed[4:], "x")
    gu0_core = [swap_core(w) for w in gu0]
    down0_core = [swap_core(w) for w in down0]

    w1 = turn(1, gate_weight, up_weight, down_weight)
    w1 = exchange(w1, "z")
    w1 = [w1[:2], w1[2:]]
    near, far = [], []
    for h in range(2):
        near.append(shift(w1[h], "x", 1))
        far.append(shift(w1[h], "x", 3))
    across = [shift(near[0], "x", 1)]
    across.append(shift(far[1], "x", 3))
    w1 = [*w1, *near, *far, *across]
    w1_core = []
    for w in w1:
        w1_core.append(swap_core(w))

    sums, next_a, next_b, over_a, over_b, prev_a, prev_b, own = gate_up(place, rows, gu0, gu0_core)
    over_a = shift(over_a, "z", 1)
    over_b = shift(over_b, "z", 3)
    next_b = shift(next_b, "z", 1)
    prev_a = shift(prev_a, "z", 3)
    next_a = shift((next_a.astype(F32) + over_a.astype(F32)).astype(BF16), "z", 1)
    prev_b = shift((prev_b.astype(F32) + over_b.astype(F32)).astype(BF16), "z", 3)
    sums = sums.astype(F32)
    sums = jnp.concatenate(
        (
            sums[: quarter // 2] + (prev_a.astype(F32) + next_a.astype(F32)),
            sums[quarter // 2 :] + (next_b.astype(F32) + prev_b.astype(F32)),
        )
    )
    hidden = (jax.nn.silu(sums[:, :cols]) * sums[:, cols:]).astype(BF16)
    hidden = share4(hidden, "z")
    partial = down(place, hidden, down0, down0_core)
    branch = exchange(partial.reshape(16, block, 1024), ("x", "y"))
    affine = in_order(mine[:, quarter : quarter + 12].astype(F32), x)
    affine = (affine[:, :4] + affine[:, 4:8]) + affine[:, 8:]
    affine = affine.transpose(1, 0, 2).reshape(4, 1024)
    spread = in_order(jnp.stack(share4(affine[::2], "z")), z)
    spread = spread.transpose(1, 0, 2).reshape(2, 4096)
    message = norm_message(in_vmem(branch), own)
    stream = in_vmem(exchange(message, ("z", "y")))

    parts, own = block_layer(place, stream, spread, w1 + w1_core)
    branch = exchange(parts, ("z", "y")).astype(F32).sum(axis=0)
    mixed = RESIDUAL * own.astype(F32) + branch
    stats = share(row_stats(mixed), "z", 4).sum(axis=0)
    out = normed(mixed, stats[0], stats[1], affine[1], affine[3])
    parts = jnp.broadcast_to(out.reshape(block, 4, 1, 256).transpose(1, 2, 0, 3), (4, 4, block, 256))
    ours = exchange(parts.reshape(16, block, 256), ("x", "y")).reshape(half, 256)
    theirs = swap_core(ours)
    return jnp.where(c == 0, jnp.concatenate((ours, theirs)), jnp.concatenate((theirs, ours)))


def solution(mesh):
    finer = Mesh(mesh.devices.reshape(4, 4, 4, 2), ("z", "x", "y", "c"))
    ra, cb = ("z", "x"), ("y", "c")
    in_specs = (
        P(None, ra),
        P(None, ra, cb),
        P(None, ra, cb),
        P(None, cb, ra),
        P(None, ra),
        P(None, ra),
    )


    return jax.shard_map(per_device, mesh=finer, in_specs=in_specs, out_specs=P(None, ra), check_vma=False)
```

```python
import jax
import jax.numpy as jnp
from jax import lax
from jax.experimental import pallas as pl
from jax.experimental.pallas import tpu as pltpu
from jax.sharding import Mesh
from jax.sharding import PartitionSpec as P

RESIDUAL = 0.5
EPSILON = 1e-05
WIDTH = 4096.0
BF16 = jnp.bfloat16
F32 = jnp.float32
ANY = pl.BlockSpec(memory_space=pltpu.HBM)
SMEM = pl.BlockSpec(memory_space=pltpu.SMEM)
VMEM = pl.BlockSpec(memory_space=pltpu.VMEM)


def exchange(parts, axes):
    return lax.all_to_all(parts, axes, 0, 0, tiled=True)


def shift(block, axis, step):
    return lax.ppermute(block, axis, [(i, (i + step) % 4) for i in range(4)])


def in_vmem(value):
    return pltpu.with_memory_space_constraint(value, pltpu.VMEM)


def swap_core(block):
    return lax.ppermute(block, "c", [(0, 1), (1, 0)])


def share4(block, axis):
    return exchange4([block] * 4, axis)


def exchange4(parts, axis):
    got = [parts[0]]
    for step in (1, 2, 3):
        got.append(shift(parts[step], axis, step))
    return got


def behind(own, k):
    return lax.rem(own + 4 - k, 4)


def dot_nt(a, b):
    return lax.dot_general(a, b, (((1,), (1,)), ((), ())), preferred_element_type=F32)


def sds(*shape):
    return jax.ShapeDtypeStruct(shape, BF16)


def run_copies(copies, sems):
    started = []
    for i, (src, dst) in enumerate(copies):
        copy = pltpu.make_async_copy(src, dst, sems.at[i])
        copy.start()
        started.append(copy)
    return started


def turn_pair(gate_ref, up_ref, turned):
    for g, ref in enumerate((gate_ref, up_ref)):
        turned[g] = ref[0].T


def turn_kernel(place_ref, gate_ref, up_ref, down_ref, *rest):
    outs, turned = rest[:-1], rest[-1]
    own = place_ref[0]
    rows = gate_ref.shape[2] // 4
    turn_pair(gate_ref, up_ref, turned)
    for k in range(4):
        at = pl.ds(pl.multiple_of(lax.rem(own + k, 4) * rows, 16), rows)
        outs[k][0:2] = turned[:, at, :]
        outs[k][2] = down_ref[0, at, :]


def turn(place, layer, gate, up, down):
    rows = gate.shape[2] // 4
    pick = lambda i: (layer, 0, 0)
    return pl.pallas_call(
        turn_kernel,
        out_shape=[sds(3, rows, 256)] * 4,
        in_specs=[
            SMEM,
            pl.BlockSpec((1, *gate.shape[1:]), pick),
            pl.BlockSpec((1, *up.shape[1:]), pick),
            pl.BlockSpec((1, *down.shape[1:]), pick),
        ],
        out_specs=[VMEM] * 4,
        grid=(1,),
        scratch_shapes=[pltpu.VMEM((2, gate.shape[2], 256), BF16)],
    )(place, gate, up, down)


def pack_kernel(place_ref, gate_ref, up_ref, down_ref, *rest):
    outs, turned = rest[:-1], rest[-1]
    own = place_ref[1]
    rows = gate_ref.shape[2] // 4
    turn_pair(gate_ref, up_ref, turned)
    for k in range(4):
        at = pl.ds(pl.multiple_of(lax.rem(own + k, 4) * rows, 16), rows)
        outs[k][0:2] = turned[:, at, :]
        outs[4 + k][...] = down_ref[0, at, :]


def pack(place, layer, gate, up, down):
    rows = gate.shape[2] // 4
    out_shape = [sds(2, rows, 256)] * 4 + [sds(rows, 256)] * 4
    pick = lambda i: (layer, 0, 0)
    return pl.pallas_call(
        pack_kernel,
        out_shape=out_shape,
        in_specs=[
            SMEM,
            pl.BlockSpec((1, *gate.shape[1:]), pick),
            pl.BlockSpec((1, *up.shape[1:]), pick),
            pl.BlockSpec((1, *down.shape[1:]), pick),
        ],
        out_specs=[VMEM] * len(out_shape),
        grid=(1,),
        scratch_shapes=[pltpu.VMEM((2, gate.shape[2], 256), BF16)],
    )(place, gate, up, down)


def gate_up_kernel(place_ref, *refs):
    rows, mine, theirs, outs, own_out = refs[:4], refs[4:8], refs[8:12], refs[12:19], refs[19]
    stream, weights, partial, sems, out_sems = refs[20:]
    z, x, y = place_ref[0], place_ref[1], place_ref[2]
    n, half = rows[0].shape[1], mine[0].shape[1]
    block = own_out.shape[0]
    lanes = [pl.ds(pl.multiple_of(behind(x, m) * 256, 256), 256) for m in range(4)]
    copies = []
    for j in range(4):
        for m in range(4):
            copies.append((rows[j].at[m], stream.at[behind(y, j), :, lanes[m]]))
    for g in range(2):
        for m in range(4):
            for s, piece in enumerate((mine[m], theirs[m])):
                at = (2 * g + s) * half
                copies.append((piece.at[g], weights.at[at : at + half, lanes[m]]))
    started = run_copies(copies, sems)
    for copy in started[:24]:
        copy.wait()
    own_out[...] = stream[x, pl.ds(pl.multiple_of(y * block, 16), block), :]
    whole = stream[...].reshape(4 * n, 1024)
    for g in range(2):
        at = slice(2 * g * half, 2 * g * half + 2 * half)
        if g == 1:
            for copy in started[24:]:
                copy.wait()
        partial[:, :, at] = dot_nt(whole, weights[at]).astype(BF16).reshape(4, n, 2 * half)
    copies = [(partial.at[z], outs[0])]
    for k in range(1, 4):
        for h in range(2):
            src = partial.at[lax.rem(z + k, 4), h * n // 2 : h * n // 2 + n // 2]
            copies.append((src, outs[2 * k - 1 + h]))
    for copy in run_copies(copies, out_sems):
        copy.wait()


def gate_up(place, rows, mine, theirs):
    n, half = rows[0].shape[1], mine[0].shape[1]
    return pl.pallas_call(
        gate_up_kernel,
        out_shape=[sds(n, 4 * half)] + [sds(n // 2, 4 * half)] * 6 + [sds(n // 4, 1024)],
        in_specs=[SMEM] + [ANY] * 12,
        out_specs=[ANY] * 7 + [VMEM],
        scratch_shapes=[
            pltpu.VMEM((4, n, 1024), BF16),
            pltpu.VMEM((4 * half, 1024), BF16),
            pltpu.VMEM((4, n, 4 * half), BF16),
            pltpu.SemaphoreType.DMA((32,)),
            pltpu.SemaphoreType.DMA((7,)),
        ],
        compiler_params=pltpu.CompilerParams(vmem_limit_bytes=56 << 20),
    )(place, *rows, *mine, *theirs)


def down_kernel(place_ref, *refs):
    hidden, mine, theirs, out = refs[:4], refs[4:8], refs[8:12], refs[12]
    rows, weights, sems = refs[13:]
    z, x = place_ref[0], place_ref[1]
    half = mine[0].shape[0]
    copies = []
    for m in range(4):
        lanes = pl.ds(pl.multiple_of(behind(x, m) * 256, 256), 256)
        copies.append((mine[m], weights.at[:half, lanes]))
        copies.append((theirs[m], weights.at[half:, lanes]))
    for k in range(4):
        copies.append((hidden[k], rows.at[behind(z, k)]))
    for copy in run_copies(copies, sems):
        copy.wait()
    n, cols = rows.shape[1:]
    out[...] = jnp.dot(rows[...].reshape(4 * n, cols), weights[...], preferred_element_type=F32).astype(BF16)


def down(place, hidden, mine, theirs):
    n, cols = hidden[0].shape
    return pl.pallas_call(
        down_kernel,
        out_shape=sds(4 * n, 1024),
        in_specs=[SMEM] + [VMEM] * 4 + [ANY] * 8,
        out_specs=VMEM,
        scratch_shapes=[
            pltpu.VMEM((4, n, cols), BF16),
            pltpu.VMEM((cols, 1024), BF16),
            pltpu.SemaphoreType.DMA((12,)),
        ],
        compiler_params=pltpu.CompilerParams(vmem_limit_bytes=24 << 20),
    )(place, *hidden, *mine, *theirs)


def parts_of(value):
    high = value.astype(BF16)
    rest = value - high.astype(F32)
    middle = rest.astype(BF16)
    return high, middle, (rest - middle.astype(F32)).astype(BF16)


def norm_kernel(branch, own, out, message, sems):
    mixed = RESIDUAL * own[...].astype(F32)
    for i in range(branch.shape[0]):
        mixed += branch[i].astype(F32)
    cols = mixed.shape[1]
    mean = mixed.sum(axis=1, keepdims=True) / cols
    mixed -= mean
    message[:, :cols] = mixed.astype(BF16)
    lane = lax.broadcasted_iota(jnp.int32, (mixed.shape[0], 128), 1)
    tail = jnp.zeros((mixed.shape[0], 128), F32)
    for i, part in enumerate(parts_of(mean) + parts_of((mixed * mixed).sum(axis=1, keepdims=True))):
        tail = jnp.where(lane == i, part.astype(F32), tail)
    message[:, cols:] = tail.astype(BF16)
    for copy in run_copies([(message, out.at[i]) for i in range(out.shape[0])], sems):
        copy.wait()


def norm_message(branch, own):
    n, cols = own.shape
    return pl.pallas_call(
        norm_kernel,
        out_shape=sds(16, n, cols + 128),
        in_specs=[VMEM] * 2,
        out_specs=ANY,
        scratch_shapes=[pltpu.VMEM((n, cols + 128), BF16), pltpu.SemaphoreType.DMA((16,))],
        compiler_params=pltpu.CompilerParams(vmem_limit_bytes=16 << 20),
    )(branch, own)


def block_kernel(place_ref, rows_ref, affine_ref, *refs):
    pieces, out, own_out = refs[:32], refs[32], refs[33]
    stream, tails, weights, hidden, row_sems, sems = refs[34:]
    z, x, y = place_ref[0], place_ref[1], place_ref[2]
    n, rows = rows_ref.shape[1], pieces[0].shape[1]
    copies = []
    for i in range(16):
        at = slice(i % 4 * n, i % 4 * n + n)
        copies.append((rows_ref.at[i, :, :1024], stream.at[at, i // 4 * 1024 : i // 4 * 1024 + 1024]))
        copies.append((rows_ref.at[i, :, 1024:], tails.at[i // 4, at]))
    row_copies = run_copies(copies, row_sems)

    def load(g):
        for i, piece in enumerate(pieces):
            at = i // 16 * rows
            lanes = pl.ds(pl.multiple_of(behind(z, i % 4) * 1024 + behind(x, i // 4 % 4) * 256, 256), 256)
            pltpu.make_async_copy(piece.at[g], weights.at[g, at : at + rows, lanes], sems.at[g]).start()

    def loaded(g):
        pltpu.make_async_copy(weights.at[g], weights.at[g], sems.at[g]).wait()

    load(0)
    for copy in row_copies:
        copy.wait()
    means, squares = [], []
    for q in range(4):
        tail = tails[q].astype(F32)
        means.append(tail[:, 0:1] + tail[:, 1:2] + tail[:, 2:3])
        squares.append(tail[:, 3:4] + tail[:, 4:5] + tail[:, 5:6])
    mean = sum(means) / 4
    square = sum(squares) + sum((m - mean) * (m - mean) for m in means) * 1024
    scale = lax.rsqrt(square / WIDTH + EPSILON)

    def normalise(q, carry):
        at = pl.ds(pl.multiple_of(q * 1024, 1024), 1024)
        tail = tails[q].astype(F32)
        offset = tail[:, 0:1] + tail[:, 1:2] + tail[:, 2:3] - mean
        value = (stream[:, at].astype(F32) + offset) * scale
        stream[:, at] = (value * affine_ref[0:1, at] + affine_ref[1:2, at]).astype(BF16)
        return carry

    lax.fori_loop(0, 4, normalise, 0)
    own_out[...] = stream[pl.ds(pl.multiple_of(y * n, 16), n), pl.ds(pl.multiple_of(z * 1024, 1024), 1024)]
    loaded(0)
    load(1)
    load(2)
    gate = dot_nt(stream[...], weights[0])
    gate = gate * jax.nn.sigmoid(gate)
    loaded(1)
    hidden[...] = (gate * dot_nt(stream[...], weights[1])).astype(BF16)
    loaded(2)

    def step(q, carry):
        lanes = pl.ds(pl.multiple_of(q * 1024, 1024), 1024)
        part = jnp.dot(hidden[...], weights[2, :, lanes], preferred_element_type=F32)
        out[pl.ds(4 * q, 4)] = part.astype(BF16).reshape(4, n, 1024)
        return carry

    lax.fori_loop(0, 4, step, 0)


def block_layer(place, rows, affine, pieces):
    n, half = rows.shape[1], pieces[0].shape[1]
    return pl.pallas_call(
        block_kernel,
        out_shape=[sds(16, n, 1024), sds(n, 1024)],
        in_specs=[SMEM, VMEM, VMEM] + [ANY] * 32,
        out_specs=[VMEM] * 2,
        scratch_shapes=[
            pltpu.VMEM((4 * n, 4096), BF16),
            pltpu.VMEM((4, 4 * n, 128), BF16),
            pltpu.VMEM((3, 2 * half, 4096), BF16),
            pltpu.VMEM((4 * n, 2 * half), BF16),
            pltpu.SemaphoreType.DMA((32,)),
            pltpu.SemaphoreType.DMA((3,)),
        ],
        compiler_params=pltpu.CompilerParams(vmem_limit_bytes=58 << 20),
    )(place, rows, affine, *pieces)


def normed(mixed, row_sum, row_squares, gain, shift_row):
    mean = row_sum / WIDTH
    var = row_squares / WIDTH - mean * mean
    out = (mixed - mean[:, None]) * lax.rsqrt(var + EPSILON)[:, None]
    return (out * gain + shift_row).astype(BF16)


def row_stats(mixed):
    return jnp.stack((mixed.sum(axis=1), (mixed * mixed).sum(axis=1)))


def in_order(pieces, own):
    back = jnp.concatenate((pieces[:1], pieces[3:4], pieces[2:3], pieces[1:2]))
    return lax.dynamic_slice_in_dim(jnp.concatenate((back, back[:3])), (4 - own) % 4, 4, 0)


def thirds(values):
    high = lax.reduce_precision(values, 8, 7)
    middle = lax.reduce_precision(values - high, 8, 7)
    low = values - high - middle
    return jnp.concatenate((high, middle, low)).astype(BF16)


def per_device(inputs, gate_weight, up_weight, down_weight, norm_gain, norm_shift):
    z, x, y, c = (lax.axis_index(a) for a in ("z", "x", "y", "c"))
    place = jnp.stack((z, x, y, c)).astype(jnp.int32)
    half = inputs.shape[0] // 2
    quarter = half // 4
    block = half // 16
    cols = gate_weight.shape[2] // 2

    mine = lax.dynamic_slice_in_dim(inputs, c * half + y * quarter, quarter, 0)
    affine = thirds(jnp.concatenate((norm_gain, norm_shift)))
    mine = jnp.concatenate((mine, affine, jnp.zeros((4, 256), BF16)))
    mine = jnp.stack(share4(mine, "x"))
    rows = share4(mine[:, :quarter], "y")

    packed = pack(place, 0, gate_weight, up_weight, down_weight)
    gu0 = exchange4(packed[:4], "x")
    down0 = exchange4(packed[4:], "x")
    gu0_core = [swap_core(w) for w in gu0]
    down0_core = [swap_core(w) for w in down0]

    w1 = turn(place, 1, gate_weight, up_weight, down_weight)
    w1 = exchange4(w1, "z")
    near, far = [], []
    for k in range(4):
        near.append(shift(w1[k], "x", 1))
        far.append(shift(w1[k], "x", 3))
    across = []
    for k in range(4):
        across.append(shift(near[k], "x", 1) if k < 2 else shift(far[k], "x", 3))
    w1 = [*w1, *near, *across, *far]
    w1_core = []
    for w in w1:
        w1_core.append(swap_core(w))

    sums, next_a, next_b, over_a, over_b, prev_a, prev_b, own = gate_up(place, rows, gu0, gu0_core)
    over_a = shift(over_a, "z", 1)
    over_b = shift(over_b, "z", 3)
    next_b = shift(next_b, "z", 1)
    prev_a = shift(prev_a, "z", 3)
    next_a = shift((next_a.astype(F32) + over_a.astype(F32)).astype(BF16), "z", 1)
    prev_b = shift((prev_b.astype(F32) + over_b.astype(F32)).astype(BF16), "z", 3)
    sums = sums.astype(F32)
    sums = jnp.concatenate(
        (
            sums[: quarter // 2] + (prev_a.astype(F32) + next_a.astype(F32)),
            sums[quarter // 2 :] + (next_b.astype(F32) + prev_b.astype(F32)),
        )
    )
    hidden = (jax.nn.silu(sums[:, :cols]) * sums[:, cols:]).astype(BF16)
    hidden = share4(hidden, "z")
    partial = down(place, [in_vmem(piece) for piece in hidden], down0, down0_core)
    branch = exchange(partial.reshape(16, block, 1024), ("x", "y"))
    affine = in_order(mine[:, quarter : quarter + 12].astype(F32), x)
    affine = (affine[:, :4] + affine[:, 4:8]) + affine[:, 8:]
    affine = affine.transpose(1, 0, 2).reshape(4, 1024)
    spread = in_order(jnp.stack(share4(affine[::2], "z")), z)
    spread = spread.transpose(1, 0, 2).reshape(2, 4096)
    message = norm_message(in_vmem(branch), own)
    stream = in_vmem(exchange(message, ("z", "y")))

    parts, own = block_layer(place, stream, spread, w1 + w1_core)
    branch = exchange(parts, ("z", "y")).astype(F32).sum(axis=0)
    mixed = RESIDUAL * own.astype(F32) + branch
    stats = share4(row_stats(mixed), "z")
    stats = (stats[0] + stats[2]) + (stats[1] + stats[3])
    out = normed(mixed, stats[0], stats[1], affine[1], affine[3])
    parts = jnp.broadcast_to(out.reshape(block, 4, 1, 256).transpose(1, 2, 0, 3), (4, 4, block, 256))
    ours = exchange(parts.reshape(16, block, 256), ("x", "y")).reshape(half, 256)
    theirs = swap_core(ours)
    return jnp.where(c == 0, jnp.concatenate((ours, theirs)), jnp.concatenate((theirs, ours)))


def solution(mesh):
    finer = Mesh(mesh.devices.reshape(4, 4, 4, 2), ("z", "x", "y", "c"))
    ra, cb = ("z", "x"), ("y", "c")
    in_specs = (
        P(None, ra),
        P(None, ra, cb),
        P(None, ra, cb),
        P(None, cb, ra),
        P(None, ra),
        P(None, ra),
    )


    return jax.shard_map(per_device, mesh=finer, in_specs=in_specs, out_specs=P(None, ra), check_vma=False)
```

```python
import jax
import jax.numpy as jnp
from jax import lax
from jax.experimental import pallas as pl
from jax.experimental.pallas import tpu as pltpu
from jax.sharding import Mesh
from jax.sharding import PartitionSpec as P

RESIDUAL = 0.5
EPSILON = 1e-05
WIDTH = 4096.0
BF16 = jnp.bfloat16
F32 = jnp.float32
ANY = pl.BlockSpec(memory_space=pltpu.HBM)
SMEM = pl.BlockSpec(memory_space=pltpu.SMEM)
VMEM = pl.BlockSpec(memory_space=pltpu.VMEM)


def exchange(parts, axes):
    return lax.all_to_all(parts, axes, 0, 0, tiled=True)


def share(block, axes, peers):
    return exchange(jnp.broadcast_to(block[None], (peers, *block.shape)), axes)


def shift(block, axis, step):
    return lax.ppermute(block, axis, [(i, (i + step) % 4) for i in range(4)])


def in_vmem(value):
    return pltpu.with_memory_space_constraint(value, pltpu.VMEM)


def swap_core(block):
    return lax.ppermute(block, "c", [(0, 1), (1, 0)])


def share4(block, axis):
    return exchange4([block] * 4, axis)


def exchange4(parts, axis):
    got = [parts[0]]
    for step in (1, 2, 3):
        got.append(shift(parts[step], axis, step))
    return got


def behind(own, k):
    return lax.rem(own + 4 - k, 4)


def dot_nt(a, b):
    return lax.dot_general(a, b, (((1,), (1,)), ((), ())), preferred_element_type=F32)


def sds(*shape):
    return jax.ShapeDtypeStruct(shape, BF16)


def run_copies(copies, sems):
    started = []
    for i, (src, dst) in enumerate(copies):
        copy = pltpu.make_async_copy(src, dst, sems.at[i])
        copy.start()
        started.append(copy)
    return started


def turn_pair(gate_ref, up_ref, turned):
    for g, ref in enumerate((gate_ref, up_ref)):
        turned[g] = ref[0].T


def turn_kernel(place_ref, gate_ref, up_ref, down_ref, *rest):
    outs, turned = rest[:-1], rest[-1]
    own = place_ref[0]
    rows = gate_ref.shape[2] // 4
    turn_pair(gate_ref, up_ref, turned)
    for k in range(4):
        at = pl.ds(pl.multiple_of(lax.rem(own + k, 4) * rows, 16), rows)
        outs[k][0:2] = turned[:, at, :]
        outs[k][2] = down_ref[0, at, :]


def turn(place, layer, gate, up, down):
    rows = gate.shape[2] // 4
    pick = lambda i: (layer, 0, 0)
    return pl.pallas_call(
        turn_kernel,
        out_shape=[sds(3, rows, 256)] * 4,
        in_specs=[
            SMEM,
            pl.BlockSpec((1, *gate.shape[1:]), pick),
            pl.BlockSpec((1, *up.shape[1:]), pick),
            pl.BlockSpec((1, *down.shape[1:]), pick),
        ],
        out_specs=[VMEM] * 4,
        grid=(1,),
        scratch_shapes=[pltpu.VMEM((2, gate.shape[2], 256), BF16)],
    )(place, gate, up, down)


def pack_kernel(place_ref, gate_ref, up_ref, down_ref, *rest):
    outs, turned = rest[:-1], rest[-1]
    own = place_ref[1]
    rows = gate_ref.shape[2] // 4
    turn_pair(gate_ref, up_ref, turned)
    for k in range(4):
        at = pl.ds(pl.multiple_of(lax.rem(own + k, 4) * rows, 16), rows)
        outs[k][0:2] = turned[:, at, :]
        outs[4 + k][...] = down_ref[0, at, :]


def pack(place, layer, gate, up, down):
    rows = gate.shape[2] // 4
    out_shape = [sds(2, rows, 256)] * 4 + [sds(rows, 256)] * 4
    pick = lambda i: (layer, 0, 0)
    return pl.pallas_call(
        pack_kernel,
        out_shape=out_shape,
        in_specs=[
            SMEM,
            pl.BlockSpec((1, *gate.shape[1:]), pick),
            pl.BlockSpec((1, *up.shape[1:]), pick),
            pl.BlockSpec((1, *down.shape[1:]), pick),
        ],
        out_specs=[VMEM] * len(out_shape),
        grid=(1,),
        scratch_shapes=[pltpu.VMEM((2, gate.shape[2], 256), BF16)],
    )(place, gate, up, down)


def gate_up_kernel(place_ref, *refs):
    rows, mine, theirs, outs, own_out = refs[:4], refs[4:8], refs[8:12], refs[12:19], refs[19]
    stream, weights, partial, sems, out_sems = refs[20:]
    z, x, y = place_ref[0], place_ref[1], place_ref[2]
    n, half = rows[0].shape[1], mine[0].shape[1]
    block = own_out.shape[0]
    lanes = [pl.ds(pl.multiple_of(behind(x, m) * 256, 256), 256) for m in range(4)]

    def slot(b):
        ahead = lax.rem(b + 4 - z, 4)
        return jnp.where(ahead == 0, 3, jnp.where(ahead == 1, 1, jnp.where(ahead == 2, 0, 2)))

    copies = []
    for j in range(4):
        for m in range(4):
            copies.append((rows[j].at[m], stream.at[slot(behind(y, j)), :, lanes[m]]))
    for g in range(2):
        for m in range(4):
            for s, piece in enumerate((mine[m], theirs[m])):
                at = (2 * g + s) * half
                copies.append((piece.at[g], weights.at[at : at + half, lanes[m]]))
    started = run_copies(copies, sems)
    for copy in started[:24]:
        copy.wait()
    own_out[...] = stream[slot(x), pl.ds(pl.multiple_of(y * block, 16), block), :]
    sent = []
    for part in range(2):
        picked = stream[2 * part : 2 * part + 2].reshape(2 * n, 1024)
        for g in range(2):
            at = slice(2 * g * half, 2 * g * half + 2 * half)
            if part == 0 and g == 1:
                for copy in started[24:]:
                    copy.wait()
            partial[2 * part : 2 * part + 2, :, at] = dot_nt(picked, weights[at]).astype(BF16).reshape(2, n, 2 * half)
        for s in (2 * part, 2 * part + 1):
            k = (2, 1, 3, 0)[s]
            if k == 0:
                copies = [(partial.at[s], outs[0])]
            else:
                copies = [(partial.at[s, h * n // 2 : h * n // 2 + n // 2], outs[2 * k - 1 + h]) for h in range(2)]
            for src, dst in copies:
                copy = pltpu.make_async_copy(src, dst, out_sems.at[len(sent)])
                copy.start()
                sent.append(copy)
    for copy in sent:
        copy.wait()


def gate_up(place, rows, mine, theirs):
    n, half = rows[0].shape[1], mine[0].shape[1]
    return pl.pallas_call(
        gate_up_kernel,
        out_shape=[sds(n, 4 * half)] + [sds(n // 2, 4 * half)] * 6 + [sds(n // 4, 1024)],
        in_specs=[SMEM] + [ANY] * 12,
        out_specs=[ANY] * 7 + [VMEM],
        scratch_shapes=[
            pltpu.VMEM((4, n, 1024), BF16),
            pltpu.VMEM((4 * half, 1024), BF16),
            pltpu.VMEM((4, n, 4 * half), BF16),
            pltpu.SemaphoreType.DMA((32,)),
            pltpu.SemaphoreType.DMA((7,)),
        ],
        compiler_params=pltpu.CompilerParams(vmem_limit_bytes=56 << 20),
    )(place, *rows, *mine, *theirs)


def down_kernel(place_ref, *refs):
    hidden, mine, theirs, out = refs[:4], refs[4:8], refs[8:12], refs[12]
    rows, weights, sems = refs[13:]
    z, x = place_ref[0], place_ref[1]
    half = mine[0].shape[0]
    copies = []
    for m in range(4):
        lanes = pl.ds(pl.multiple_of(behind(x, m) * 256, 256), 256)
        copies.append((mine[m], weights.at[:half, lanes]))
        copies.append((theirs[m], weights.at[half:, lanes]))
    for k in range(4):
        copies.append((hidden[k], rows.at[behind(z, k)]))
    for copy in run_copies(copies, sems):
        copy.wait()
    n, cols = rows.shape[1:]
    out[...] = jnp.dot(rows[...].reshape(4 * n, cols), weights[...], preferred_element_type=F32).astype(BF16)


def down(place, hidden, mine, theirs):
    n, cols = hidden[0].shape
    return pl.pallas_call(
        down_kernel,
        out_shape=sds(4 * n, 1024),
        in_specs=[SMEM] + [VMEM] * 4 + [ANY] * 8,
        out_specs=VMEM,
        scratch_shapes=[
            pltpu.VMEM((4, n, cols), BF16),
            pltpu.VMEM((cols, 1024), BF16),
            pltpu.SemaphoreType.DMA((12,)),
        ],
        compiler_params=pltpu.CompilerParams(vmem_limit_bytes=24 << 20),
    )(place, *hidden, *mine, *theirs)


def parts_of(value):
    high = value.astype(BF16)
    rest = value - high.astype(F32)
    middle = rest.astype(BF16)
    return high, middle, (rest - middle.astype(F32)).astype(BF16)


def norm_kernel(branch, own, out, message):
    mixed = RESIDUAL * own[...].astype(F32)
    for i in range(branch.shape[0]):
        mixed += branch[i].astype(F32)
    cols = mixed.shape[1]
    mean = mixed.sum(axis=1, keepdims=True) / cols
    mixed -= mean
    message[:, :cols] = mixed.astype(BF16)
    lane = lax.broadcasted_iota(jnp.int32, (mixed.shape[0], 128), 1)
    tail = jnp.zeros((mixed.shape[0], 128), F32)
    for i, part in enumerate(parts_of(mean) + parts_of((mixed * mixed).sum(axis=1, keepdims=True))):
        tail = jnp.where(lane == i, part.astype(F32), tail)
    message[:, cols:] = tail.astype(BF16)
    whole = message[...]
    for i in range(out.shape[0]):
        out[i] = whole


def norm_message(branch, own):
    n, cols = own.shape
    return pl.pallas_call(
        norm_kernel,
        out_shape=sds(16, n, cols + 128),
        in_specs=[VMEM] * 2,
        out_specs=VMEM,
        scratch_shapes=[pltpu.VMEM((n, cols + 128), BF16)],
        compiler_params=pltpu.CompilerParams(vmem_limit_bytes=16 << 20),
    )(branch, own)


def block_kernel(place_ref, rows_ref, affine_ref, *refs):
    pieces, out, own_out = refs[:32], refs[32], refs[33]
    stream, tails, weights, hidden, row_sems, sems = refs[34:]
    z, x, y = place_ref[0], place_ref[1], place_ref[2]
    n, rows = rows_ref.shape[1], pieces[0].shape[1]
    copies = []
    for i in range(16):
        at = slice(i % 4 * n, i % 4 * n + n)
        copies.append((rows_ref.at[i, :, :1024], stream.at[at, i // 4 * 1024 : i // 4 * 1024 + 1024]))
        copies.append((rows_ref.at[i, :, 1024:], tails.at[i // 4, at]))
    row_copies = run_copies(copies, row_sems)

    def load(g):
        for i, piece in enumerate(pieces):
            at = i // 16 * rows
            lanes = pl.ds(pl.multiple_of(behind(z, i % 4) * 1024 + behind(x, i // 4 % 4) * 256, 256), 256)
            pltpu.make_async_copy(piece.at[g], weights.at[g, at : at + rows, lanes], sems.at[g]).start()

    def loaded(g):
        pltpu.make_async_copy(weights.at[g], weights.at[g], sems.at[g]).wait()

    load(0)
    load(1)
    for copy in row_copies:
        copy.wait()
    means, squares = [], []
    for q in range(4):
        tail = tails[q].astype(F32)
        means.append(tail[:, 0:1] + tail[:, 1:2] + tail[:, 2:3])
        squares.append(tail[:, 3:4] + tail[:, 4:5] + tail[:, 5:6])
    mean = sum(means) / 4
    square = sum(squares) + sum((m - mean) * (m - mean) for m in means) * 1024
    scale = lax.rsqrt(square / WIDTH + EPSILON)

    def normalise(q, carry):
        at = pl.ds(pl.multiple_of(q * 1024, 1024), 1024)
        tail = tails[q].astype(F32)
        offset = tail[:, 0:1] + tail[:, 1:2] + tail[:, 2:3] - mean
        value = (stream[:, at].astype(F32) + offset) * scale
        stream[:, at] = (value * affine_ref[0:1, at] + affine_ref[1:2, at]).astype(BF16)
        return carry

    lax.fori_loop(0, 4, normalise, 0)
    own_out[...] = stream[pl.ds(pl.multiple_of(y * n, 16), n), pl.ds(pl.multiple_of(z * 1024, 1024), 1024)]
    load(2)
    loaded(0)
    gate = dot_nt(stream[...], weights[0])
    gate = gate * jax.nn.sigmoid(gate)
    loaded(1)
    hidden[...] = (gate * dot_nt(stream[...], weights[1])).astype(BF16)
    loaded(2)

    def step(q, carry):
        lanes = pl.ds(pl.multiple_of(q * 1024, 1024), 1024)
        part = jnp.dot(hidden[...], weights[2, :, lanes], preferred_element_type=F32)
        out[pl.ds(4 * q, 4)] = part.astype(BF16).reshape(4, n, 1024)
        return carry

    lax.fori_loop(0, 4, step, 0)


def block_layer(place, rows, affine, pieces):
    n, half = rows.shape[1], pieces[0].shape[1]
    return pl.pallas_call(
        block_kernel,
        out_shape=[sds(16, n, 1024), sds(n, 1024)],
        in_specs=[SMEM, VMEM, VMEM] + [ANY] * 32,
        out_specs=[VMEM] * 2,
        scratch_shapes=[
            pltpu.VMEM((4 * n, 4096), BF16),
            pltpu.VMEM((4, 4 * n, 128), BF16),
            pltpu.VMEM((3, 2 * half, 4096), BF16),
            pltpu.VMEM((4 * n, 2 * half), BF16),
            pltpu.SemaphoreType.DMA((32,)),
            pltpu.SemaphoreType.DMA((3,)),
        ],
        compiler_params=pltpu.CompilerParams(vmem_limit_bytes=58 << 20),
    )(place, rows, affine, *pieces)


def normed(mixed, row_sum, row_squares, gain, shift_row):
    mean = row_sum / WIDTH
    var = row_squares / WIDTH - mean * mean
    out = (mixed - mean[:, None]) * lax.rsqrt(var + EPSILON)[:, None]
    return (out * gain + shift_row).astype(BF16)


def row_stats(mixed):
    return jnp.stack((mixed.sum(axis=1), (mixed * mixed).sum(axis=1)))


def in_order(pieces, own):
    back = jnp.concatenate((pieces[:1], pieces[3:4], pieces[2:3], pieces[1:2]))
    return lax.dynamic_slice_in_dim(jnp.concatenate((back, back[:3])), (4 - own) % 4, 4, 0)


def thirds(values):
    high = lax.reduce_precision(values, 8, 7)
    middle = lax.reduce_precision(values - high, 8, 7)
    low = values - high - middle
    return jnp.concatenate((high, middle, low)).astype(BF16)


def per_device(inputs, gate_weight, up_weight, down_weight, norm_gain, norm_shift):
    z, x, y, c = (lax.axis_index(a) for a in ("z", "x", "y", "c"))
    place = jnp.stack((z, x, y, c)).astype(jnp.int32)
    half = inputs.shape[0] // 2
    quarter = half // 4
    block = half // 16
    cols = gate_weight.shape[2] // 2

    mine = lax.dynamic_slice_in_dim(inputs, c * half + y * quarter, quarter, 0)
    affine = thirds(jnp.concatenate((norm_gain, norm_shift)))
    mine = jnp.concatenate((mine, affine, jnp.zeros((4, 256), BF16)))
    mine = jnp.stack(share4(mine, "x"))
    rows = share4(mine[:, :quarter], "y")

    packed = pack(place, 0, gate_weight, up_weight, down_weight)
    gu0 = exchange4(packed[:4], "x")
    down0 = exchange4(packed[4:], "x")
    gu0_core = [swap_core(w) for w in gu0]
    down0_core = [swap_core(w) for w in down0]

    w1 = turn(place, 1, gate_weight, up_weight, down_weight)
    w1 = exchange4(w1, "z")
    near, far = [], []
    for k in range(4):
        near.append(shift(w1[k], "x", 1))
        far.append(shift(w1[k], "x", 3))
    across = []
    for k in range(4):
        across.append(shift(near[k], "x", 1) if k < 2 else shift(far[k], "x", 3))
    w1 = [*w1, *near, *across, *far]
    w1_core = []
    for w in w1:
        w1_core.append(swap_core(w))

    sums, next_a, next_b, over_a, over_b, prev_a, prev_b, own = gate_up(place, rows, gu0, gu0_core)
    over_a = shift(over_a, "z", 1)
    over_b = shift(over_b, "z", 3)
    next_b = shift(next_b, "z", 1)
    prev_a = shift(prev_a, "z", 3)
    next_a = shift((next_a.astype(F32) + over_a.astype(F32)).astype(BF16), "z", 1)
    prev_b = shift((prev_b.astype(F32) + over_b.astype(F32)).astype(BF16), "z", 3)
    sums = sums.astype(F32)
    sums = jnp.concatenate(
        (
            sums[: quarter // 2] + (prev_a.astype(F32) + next_a.astype(F32)),
            sums[quarter // 2 :] + (next_b.astype(F32) + prev_b.astype(F32)),
        )
    )
    hidden = (jax.nn.silu(sums[:, :cols]) * sums[:, cols:]).astype(BF16)
    hidden = share4(hidden, "z")
    partial = down(place, [in_vmem(piece) for piece in hidden], down0, down0_core)
    branch = exchange(partial.reshape(16, block, 1024), ("x", "y"))
    affine = in_order(mine[:, quarter : quarter + 12].astype(F32), x)
    affine = (affine[:, :4] + affine[:, 4:8]) + affine[:, 8:]
    affine = affine.transpose(1, 0, 2).reshape(4, 1024)
    spread = in_order(jnp.stack(share4(affine[::2], "z")), z)
    spread = spread.transpose(1, 0, 2).reshape(2, 4096)
    message = norm_message(in_vmem(branch), own)
    stream = in_vmem(exchange(message, ("z", "y")))

    parts, own = block_layer(place, stream, spread, w1 + w1_core)
    branch = exchange(parts, ("z", "y")).astype(F32).sum(axis=0)
    mixed = RESIDUAL * own.astype(F32) + branch
    stats = share(row_stats(mixed), "z", 4).sum(axis=0)
    out = normed(mixed, stats[0], stats[1], affine[1], affine[3])
    parts = jnp.broadcast_to(out.reshape(block, 4, 1, 256).transpose(1, 2, 0, 3), (4, 4, block, 256))
    ours = exchange(parts.reshape(16, block, 256), ("x", "y")).reshape(half, 256)
    theirs = swap_core(ours)
    whole = lax.dynamic_update_slice_in_dim(jnp.zeros((2 * half, 256), BF16), ours, c * half, 0)
    return lax.dynamic_update_slice_in_dim(whole, theirs, (1 - c) * half, 0)


def solution(mesh):
    finer = Mesh(mesh.devices.reshape(4, 4, 4, 2), ("z", "x", "y", "c"))
    ra, cb = ("z", "x"), ("y", "c")
    in_specs = (
        P(None, ra),
        P(None, ra, cb),
        P(None, ra, cb),
        P(None, cb, ra),
        P(None, ra),
        P(None, ra),
    )


    return jax.shard_map(per_device, mesh=finer, in_specs=in_specs, out_specs=P(None, ra), check_vma=False)
```
